32 devices in a mesh: ep: 8 (over z, core), tp: 4 (over y, x).
Axes of the slice: x: 2, y: 2, z: 4, core: 2. Of those that a mesh axis runs over, the one named last changes fastest.
Arguments:
- tokens: bfloat16 [256, 4096], P('ep', 'tp'), may hold values from -256 to 256
- expert_ids: int32 [256, 8], P('ep'), may hold values from 0 to 15, all different within a row; in each aligned block of 32 rows (0 to 31, 32 to 63, ...) at most 32 rows name the same one
- route_weights: float32 [256, 8], P('ep'), may hold values from 0.05 to 1
- gain_in: float32 [4096], P('tp'), may hold values from 0.1 to 1.9
- gain_out: float32 [4096], P('tp'), may hold values from 0.1 to 1.9
- gate_weights: bfloat16 [16, 4096, 1024], P('ep', 'tp'), may hold values from -0.09375 to 0.09375
- up_weights: bfloat16 [16, 4096, 1024], P('ep', 'tp'), may hold values from -0.09375 to 0.09375
- down_weights: bfloat16 [16, 1024, 4096], P('ep', None, 'tp'), may hold values from -0.1875 to 0.1875
Outputs:
- mixed: bfloat16 [256, 4096], P('ep', 'tp')
The draws below stay inside these ranges and needn't reach their ends.
Inputs may be any that keep to these rules, and one draw needn't show every extreme that they name: `expert_ids`: each row names 8 different experts. Within the rows of one index of ep (aligned blocks of 32 rows) no expert is named more than 32 times, and in some blocks some expert is named exactly 32 times.
All inputs are finite; a program needn't handle non-finite values.
Results may differ from the reference program's by a relative error of at most 0.023.
Values may be sent and summed in bfloat16 or wider, within the bound.
A program may use at most 64 MiB of HBM per device.

```python
import math
import jax
import jax.numpy as jnp
import numpy as np
from jax import lax

D = 4096
FF = 1024
TOPK = 8
TOK_DEV = 32
EXPERTS = 16
TOKENS = 256
CAP = 32
N_EP = 8
N_TP = 4


def draw_tokens(key, part):
    base_key, column_key, row_key = jax.random.split(jax.random.fold_in(key, 17), 3)
    block_of = (jnp.arange(D) // (D // N_TP)).astype(jnp.float32)
    position = block_of / max(N_TP - 1, 1)
    entries = jnp.clip(jax.random.normal(base_key, (TOKENS, D), jnp.float32), -4.0, 4.0)
    rising = 3.0 ** position
    roughness = jax.random.uniform(column_key, (D,), jnp.float32, 0.5, 1.5)
    row_scale = jnp.exp(jax.random.uniform(row_key, (TOKENS, 1), jnp.float32, 0.0, 2.3))
    return (entries * (rising * roughness)[None, :] * row_scale).astype(jnp.bfloat16)


def block_scale(rng, dims, cuts, least, top_value):
    def one(dim, shards_of):
        steps = jax.random.uniform(jax.random.fold_in(jax.random.fold_in(rng, 6), dim), (shards_of,), jnp.float32, least / len(cuts), top_value / len(cuts))
        return jnp.repeat(jnp.exp(steps), dims[dim] // shards_of).reshape((-1,) + (1,) * (len(dims) - dim - 1))

    level = one(*cuts[0])
    for cut in cuts[1:]:
        level = level * one(*cut)
    return level


def deal_out(rng, own, number, rows, number_of, top, bound, slope):
    sequence = jax.random.permutation(rng, number_of)
    heavy_load, common = portions_of(number_of, rows * top, bound, slope, True), portions_of(number_of, rows * top, bound, slope, False)
    places = jnp.arange(number_of)

    def named(lengths, offset_by):
        used = int((lengths > 0).sum())
        fixed = max(1, used // 4)
        shifted = fixed + (places - fixed + offset_by * (used - fixed)) % max(1, number_of - fixed)
        return jnp.zeros((number_of,), jnp.int32).at[sequence[jnp.where(places < fixed, places, shifted)]].set(jnp.asarray(lengths, jnp.int32))

    lengths = jnp.where(number % 4 == 0, named(heavy_load, number // 4), named(common, number - number // 4 - 1))
    mixed = jax.random.permutation(jax.random.fold_in(own, 3), number_of)
    giver, sink = mixed[0:number_of // 2 * 2:2], mixed[1:number_of // 2 * 2:2]
    margin = jnp.minimum(lengths[giver] - 1, bound - lengths[sink]) // 2
    margin = jnp.where((giver == sequence[0]) | (sink == sequence[0]) | (lengths[sink] == 0), 0, jnp.maximum(margin, 0))
    shifted = jax.random.randint(jax.random.fold_in(own, 4), (number_of // 2,), 0, 1 << 20) % (margin + 1)
    lengths = lengths.at[giver].add(-shifted).at[sink].add(shifted)
    members = jnp.searchsorted(jnp.cumsum(lengths), jnp.arange(rows * top), side="right").astype(jnp.int32)
    table = members.reshape(top, rows).T
    table = table[jax.random.permutation(jax.random.fold_in(own, 1), rows)]
    offset_by = jax.random.randint(jax.random.fold_in(own, 2), (rows, 1), 0, top)
    return jnp.take_along_axis(table, (jnp.arange(top)[None, :] + offset_by) % top, axis=1)


def portions_of(amount, total, limit, skew, full):
    loads = [(1 << 20) // math.isqrt(grade ** skew) + 1 for grade in range(1, amount + 1)]
    largest = limit if full else min(limit, max(-(-total // amount), total * loads[0] // sum(loads)))
    least = 1 if total - largest >= amount - 1 else 0
    given, surplus = [largest] + [least] * (amount - 1), total - largest - least * (amount - 1)
    while surplus > 0:
        free = [i for i in range(1, amount) if given[i] < largest] or [i for i in range(1, amount) if given[i] < limit]
        pool, budget = sum([loads[i] for i in free]), surplus
        for i in free:
            extra = min(limit - given[i], max(1, budget * loads[i] // pool), surplus)
            given[i] = given[i] + extra
            surplus = surplus - extra
    return np.array(given)


def noise(own_key, dims, deviation, most, cuts=(), kind=jnp.bfloat16):
    drawn = jax.random.normal(own_key, dims, jnp.float32) * deviation
    if len(cuts) > 0:
        drawn = block_scale(own_key, dims, cuts, -0.22, 0.18) * drawn
    return jnp.clip(drawn, min=-most, max=most).astype(kind)


def setup_inputs(seed: int = 0) -> dict:
    arg_keys = jax.random.split(jax.random.key(seed), 9)
    tokens = draw_tokens(jax.random.fold_in(arg_keys[8], 71), 0)
    expert_ids_keys = jax.random.split(jax.random.fold_in(arg_keys[1], 1), TOKENS // TOK_DEV)
    expert_ids_turns = jax.random.permutation(jax.random.fold_in(arg_keys[1], 3), TOKENS // TOK_DEV)
    expert_ids = jax.vmap(lambda own, number: deal_out(jax.random.fold_in(arg_keys[1], 2), own, number, TOK_DEV, EXPERTS, TOPK, CAP, 2))(expert_ids_keys, expert_ids_turns).reshape((TOKENS, TOPK))
    route_weights = jnp.clip(jnp.exp(math.log(1.0) - 2.9957323 * jax.random.uniform(arg_keys[2], (TOKENS, TOPK), jnp.float32) ** block_scale(arg_keys[2], (TOKENS, TOPK), ((0, 8),), -0.2, 0.2)), 0.05, 1.0)
    gain_in = jnp.clip(1.0 + 0.18 * jax.random.normal(arg_keys[3], (D,), jnp.float32), 0.1, 1.9)
    gain_out = jnp.clip(1.0 + 0.18 * jax.random.normal(arg_keys[4], (D,), jnp.float32), 0.1, 1.9)
    gate_weights = noise(arg_keys[5], (EXPERTS, D, FF), D ** -0.5, 0.09375, ((0, 8), (1, 4)))
    up_weights = noise(arg_keys[6], (EXPERTS, D, FF), D ** -0.5, 0.09375, ((0, 8), (1, 4)))
    down_weights = noise(arg_keys[7], (EXPERTS, FF, D), FF ** -0.5, 0.1875, ((0, 8), (2, 4)))
    return dict(tokens=tokens, expert_ids=expert_ids, route_weights=route_weights, gain_in=gain_in, gain_out=gain_out, gate_weights=gate_weights, up_weights=up_weights, down_weights=down_weights)


epsilon = 1e-06

def blocked_product(expert_rows, weight_block):
    pieces = jnp.einsum('rbd,bdf->brf', expert_rows.reshape(expert_rows.shape[0], N_TP, D // N_TP).astype(jnp.float32), weight_block.reshape(N_TP, D // N_TP, FF).astype(jnp.float32))
    rounded = lax.optimization_barrier(pieces.astype(jnp.bfloat16))
    return lax.optimization_barrier(jnp.sum(rounded.astype(jnp.float32), axis=0))

def expert_output(operands):
    expert_rows, gate_weight, up_weight, down_weight = operands
    gate_sum = blocked_product(expert_rows, gate_weight)
    up_sum = blocked_product(expert_rows, up_weight)
    hidden = (jax.nn.silu(gate_sum) * up_sum).astype(jnp.bfloat16)
    return jnp.dot(hidden, down_weight, preferred_element_type=jnp.float32).astype(jnp.bfloat16)

def reference(tokens, expert_ids, route_weights, gain_in, gain_out, gate_weights, up_weights, down_weights):
    widened = tokens.astype(jnp.float32)
    normed = (widened * lax.rsqrt(lax.optimization_barrier(jnp.mean(widened * widened, axis=1, keepdims=True)) + epsilon) * gain_in[None, :]).astype(jnp.bfloat16)
    pair_ids = expert_ids.reshape(N_EP, TOK_DEV * TOPK)
    expert_hot = (pair_ids[:, :, None] == jnp.arange(EXPERTS, dtype=jnp.int32)[None, None, :]).astype(jnp.int32)
    slot_rank = lax.optimization_barrier(jnp.sum((jnp.cumsum(expert_hot, axis=1) - 1) * expert_hot, axis=2))
    sources = jnp.arange(N_EP, dtype=jnp.int32)[:, None]
    slot_ids = (pair_ids * (N_EP * CAP) + sources * CAP + slot_rank).reshape(-1).astype(jnp.int32)
    pair_rows = jnp.repeat(normed, TOPK, axis=0)
    slot_table = jnp.zeros((EXPERTS * N_EP * CAP, D), jnp.bfloat16).at[slot_ids].set(pair_rows)
    outputs = lax.map(expert_output, (slot_table.reshape(EXPERTS, N_EP * CAP, D), gate_weights, up_weights, down_weights))
    picked = outputs.reshape(EXPERTS * N_EP * CAP, D)[slot_ids].reshape(TOKENS, TOPK, D).astype(jnp.float32)
    combined = lax.optimization_barrier(jnp.sum(picked * route_weights[:, :, None], axis=1))
    scale = lax.rsqrt(lax.optimization_barrier(jnp.mean(combined * combined, axis=1, keepdims=True)) + epsilon)
    return (combined * scale * gain_out[None, :]).astype(jnp.bfloat16)
```

```python
import jax
import jax.numpy as jnp
from jax import lax
from jax.experimental import pallas as pl
from jax.experimental.pallas import tpu as pltpu
from jax.sharding import PartitionSpec as P

D = 4096


epsilon = 1e-06


def expert_apply(incoming, gate_weights, up_weights, down_weights):
    gate_part = jnp.einsum(
        "secd,edf->secf", incoming, gate_weights, preferred_element_type=jnp.float32
    ).astype(jnp.bfloat16)
    up_part = jnp.einsum(
        "secd,edf->secf", incoming, up_weights, preferred_element_type=jnp.float32
    ).astype(jnp.bfloat16)
    gate_sum, up_sum = (
        lax.psum(gate_part, "tp").astype(jnp.float32),
        lax.psum(up_part, "tp").astype(jnp.float32),
    )
    hidden = (jax.nn.silu(gate_sum) * up_sum).astype(jnp.bfloat16)
    total = jnp.einsum("secf,efd->secd", hidden, down_weights, preferred_element_type=jnp.float32)
    return total.astype(jnp.bfloat16)


def on_device(
    tokens, expert_ids, route_weights, gain_in, gain_out, gate_weights, up_weights, down_weights
):
    tok_count, local_width = tokens.shape
    top_count = expert_ids.shape[1]
    local_experts = gate_weights.shape[0]
    ep_count = lax.axis_size("ep")
    all_experts = local_experts * ep_count
    capacity = max(2, 2 * tok_count * top_count // all_experts)
    widened = tokens.astype(jnp.float32)
    squares = lax.psum(jnp.sum(widened * widened, axis=1), "tp")
    normed = (widened * lax.rsqrt(squares / D + epsilon)[:, None] * gain_in[None, :]).astype(
        jnp.bfloat16
    )
    pair_ids = expert_ids.reshape(-1)
    expert_hot = (pair_ids[:, None] == jnp.arange(all_experts, dtype=jnp.int32)[None, :]).astype(
        jnp.int32
    )
    slot_rank = jnp.sum((jnp.cumsum(expert_hot, axis=0) - 1) * expert_hot, axis=1)
    slot_ids = pair_ids * capacity + slot_rank
    slot_hot = (
        slot_ids[:, None] == jnp.arange(all_experts * capacity, dtype=jnp.int32)[None, :]
    ).astype(jnp.float32)
    pair_rows = jnp.repeat(normed, top_count, axis=0)
    outgoing = jnp.einsum(
        "ps,pd->sd", slot_hot.astype(jnp.bfloat16), pair_rows, preferred_element_type=jnp.float32
    ).astype(jnp.bfloat16)
    incoming = lax.all_to_all(
        outgoing.reshape(ep_count, local_experts, capacity, local_width),
        "ep",
        split_axis=0,
        concat_axis=0,
        tiled=True,
    )
    results = expert_apply(incoming, gate_weights, up_weights, down_weights)
    returned = lax.all_to_all(results, "ep", split_axis=0, concat_axis=0, tiled=True)
    weighting = jnp.sum(
        (slot_hot * route_weights.reshape(-1)[:, None]).reshape(tok_count, top_count, -1), axis=1
    )
    combined = jnp.dot(
        weighting,
        returned.reshape(-1, local_width).astype(jnp.float32),
        precision=lax.Precision.HIGHEST,
    )
    out_squares = lax.psum(jnp.sum(combined * combined, axis=1), "tp")
    return (combined * lax.rsqrt(out_squares / D + epsilon)[:, None] * gain_out[None, :]).astype(
        jnp.bfloat16
    )


MESH = pl.DeviceIdType.MESH
BF16, F32 = jnp.bfloat16, jnp.float32


def remote(src, dst, send_sem, recv_sem, target):
    return pltpu.make_async_remote_copy(
        src_ref=src,
        dst_ref=dst,
        send_sem=send_sem,
        recv_sem=recv_sem,
        device_id=target,
        device_id_type=MESH,
    )


def chip_at(z, k):
    low = lax.rem(lax.rem(z, 2) + lax.rem(k, 2), 2)
    high = lax.rem(z // 2 + k // 2, 2)
    return high * 2 + low


def dense_kernel(
    x_ref, ids_ref, rw_ref, gi_ref, go_ref, gate_hbm, up_hbm, down_hbm, o_ref,
    w0, w1, dw, xg, xs, ssb, sst, scale, wr, sbuf, r1, s2, r2, keep, hid,
    acc, dsend, drecv, zsend, zrecv, sq,
    wsem, ag_s, ag_r, fw_s, fw_r, ss_s, ss_r, p1_s, p1_r, p2_s, p2_r, p3_s, p3_r,
    p4_s, p4_r, d_s, d_r, z_s, z_r, q_s, q_r,
):
    rows, width = x_ref.shape
    chunks = xg.shape[0]
    half = w0.shape[3]
    quarter = half // 2
    lanes = ssb.shape[2]
    ep, tp = lax.axis_index("ep"), lax.axis_index("tp")
    z, c = ep // 2, lax.rem(ep, 2)
    y, x = tp // 2, lax.rem(tp, 2)
    xn, yn, dn = y * 2 + 1 - x, (1 - y) * 2 + x, (1 - y) * 2 + 1 - x
    other = z * 2 + 1 - c
    first = ((ep, xn), (ep, yn))
    second = ((ep, yn), (ep, xn))
    big, small = (x, y), (y, x)
    planes = ((ep, xn), (ep, yn), (ep, dn))

    mats = (gate_hbm, up_hbm)
    load0, load1, load2 = [], [], []
    for e in range(2):
        for m in range(2):
            off = pl.multiple_of((1 - big[e]) * half, quarter)
            load0.append(pltpu.make_async_copy(
                mats[m].at[e, :, pl.ds(off, half)], w0.at[e, m], wsem.at[e * 2 + m]))
            for s in range(2):
                q = small[e] if s else 1 - small[e]
                off = pl.multiple_of(big[e] * half + q * quarter, quarter)
                load1.append(pltpu.make_async_copy(
                    mats[m].at[e, :, pl.ds(off, quarter)], w1.at[e, m, s],
                    wsem.at[4 + e * 4 + m * 2 + s]))
        load2.append(pltpu.make_async_copy(down_hbm.at[e], dw.at[e], wsem.at[12 + e]))
    for load in load0:
        load.start()

    lane = lax.broadcasted_iota(jnp.int32, (rows, lanes), 1)
    ids, rw = ids_ref[...], rw_ref[...]
    route = jnp.zeros((rows, lanes), F32)
    for k in range(ids.shape[1]):
        hit = (ids[:, k : k + 1] == lane) | (ids[:, k : k + 1] == lane - lanes // 2)
        route = route + jnp.where(hit, rw[:, k : k + 1], 0.0)
    high = route.astype(BF16)
    low = (route - high.astype(F32)).astype(BF16)
    xg[0, c, :, :width] = x_ref[...]
    xg[0, c, :, width:] = jnp.where(
        lane < lanes // 2, high.astype(F32), low.astype(F32)
    ).astype(BF16)

    barrier = pltpu.get_barrier_semaphore()
    greet = [(other, tp)] + [(chip_at(z, k) * 2 + c, tp) for k in range(1, chunks)] + list(planes)
    for target in greet:
        pl.semaphore_signal(barrier, inc=1, device_id=target, device_id_type=MESH)
    pl.semaphore_wait(barrier, len(greet))

    def gather(k):
        return remote(xg.at[0, c], xg.at[k, c], ag_s.at[k], ag_r.at[k], (chip_at(z, k) * 2 + c, tp))

    def forward(k):
        return remote(xg.at[k, c], xg.at[k, c], fw_s.at[k], fw_r.at[k], (other, tp))

    forward(0).start()
    for k in range(1, chunks):
        gather(k).start()
    for load in load1 + load2:
        load.start()

    gain = gi_ref[...]
    for load in load0:
        load.wait()

    def phase1(k, e):
        return remote(sbuf.at[k, e], r1.at[k, e], p1_s.at[k, e], p1_r.at[k, e], first[e])

    def phase2(k, e):
        return remote(s2.at[k, e], r2.at[k, e], p2_s.at[k, e], p2_r.at[k, e], second[e])

    def phase3(k, e):
        block = hid.at[k, e, big[e] * 2 + small[e]]
        return remote(block, block, p3_s.at[k, e], p3_r.at[k, e], second[e])

    def phase4(k, e):
        block = hid.at[k, e, pl.ds(big[e] * 2, 2)]
        return remote(block, block, p4_s.at[k, e], p4_r.at[k, e], first[e])

    def across(k):
        return remote(dsend.at[k], drecv.at[k], d_s.at[k], d_r.at[k], (other, tp))

    def home(k):
        return remote(zsend.at[k], zrecv.at[k], z_s.at[k], z_r.at[k], (chip_at(z, k) * 2 + c, tp))

    @pl.loop(0, chunks)
    def _(k):
        @pl.when(k > 0)
        def _():
            gather(k).wait_recv()
            forward(k).start()

        forward(k).wait_recv()
        for j in range(2):
            at = pl.ds(j * rows, rows)
            xf = xg[k, j, :, :width].astype(F32)
            ssb[k, at, :] = jnp.broadcast_to(
                jnp.sum(xf * xf, axis=1, keepdims=True), (rows, lanes))
            xs[k, at, :] = (xf * gain).astype(BF16)
            r = xg[k, j, :, width:].astype(F32)
            for e in range(2):
                mine = ep * 2 + e
                hit = (lane == mine) | (lane == mine + lanes // 2)
                wr[k, e, at, :] = jnp.broadcast_to(
                    jnp.sum(jnp.where(hit, r, 0.0), axis=1, keepdims=True), (rows, lanes))
        for e in range(2):
            for m in range(2):
                p = jnp.dot(xs[k], w0[e, m], preferred_element_type=F32).astype(BF16)
                sbuf[k, e, m, 0] = p[:, :quarter]
                sbuf[k, e, m, 1] = p[:, quarter:]
            phase1(k, e).start()

    def squares(i):
        return remote(sst.at[0], sst.at[i], ss_s.at[i], ss_r.at[i], planes[i - 1])

    sst[0] = jnp.transpose(ssb[...].reshape(chunks * 2 * rows, lanes))[:8]
    for i in range(1, 4):
        squares(i).start()
    for load in load1:
        load.wait()

    def order(i):
        return lax.rem(i + 1, chunks)

    @pl.loop(0, chunks)
    def _(i):
        k = order(i)
        for e in range(2):
            phase1(k, e).wait_recv()
            for m in range(2):
                p = jnp.dot(xs[k], w1[e, m, 0], preferred_element_type=F32)
                s2[k, e, m] = (p + r1[k, e, m, 1 - small[e]].astype(F32)).astype(BF16)
            phase2(k, e).start()
            for m in range(2):
                p = jnp.dot(xs[k], w1[e, m, 1], preferred_element_type=F32)
                keep[k, e, m] = p + r1[k, e, m, small[e]].astype(F32)

    for i in range(1, 4):
        squares(i).wait_recv()
    total = jnp.sum(sst[...], axis=0)
    total = jnp.transpose(jnp.concatenate([total] * (lanes // 8), axis=0))
    scale[...] = lax.rsqrt(total / D + epsilon).reshape(scale.shape)
    for load in load2:
        load.wait()

    @pl.loop(0, chunks + 3)
    def _(i):
        @pl.when(i < chunks)
        def _():
            k = order(i)
            s = jnp.concatenate([scale[k]] * (quarter // lanes), axis=1)
            for e in range(2):
                phase2(k, e).wait_recv()
                g = (keep[k, e, 0] + r2[k, e, 0].astype(F32)) * s
                u = (keep[k, e, 1] + r2[k, e, 1].astype(F32)) * s
                w = jnp.concatenate([wr[k, e]] * (quarter // lanes), axis=1)
                h = g / (1.0 + jnp.exp(-g)) * u * w
                hid[k, e, big[e] * 2 + small[e]] = h.astype(BF16)
                phase3(k, e).start()

        @pl.when((i >= 1) & (i < chunks + 1))
        def _():
            k = order(i - 1)
            for e in range(2):
                phase3(k, e).wait_recv()
                phase4(k, e).start()

        @pl.when((i >= 2) & (i < chunks + 2))
        def _():
            k = order(i - 2)
            for e in range(2):
                phase4(k, e).wait_recv()
            hcat = jnp.concatenate([hid[k, e, q] for e in range(2) for q in range(4)], axis=1)
            for n in range(0, width, half):
                cols = pl.ds(n, half)
                down = jnp.concatenate([dw[0, :, cols], dw[1, :, cols]], axis=0)
                p = jnp.dot(hcat, down, preferred_element_type=F32)
                acc[k, 0, :, cols] = p[:rows]
                acc[k, 1, :, cols] = p[rows:]
            dsend[k] = acc[k, 1 - c].astype(BF16)
            across(k).start()

        @pl.when((i >= 3) & (i < chunks + 2))
        def _():
            k = order(i - 3)
            across(k).wait_recv()
            zsend[k] = (acc[k, c] + drecv[k].astype(F32)).astype(BF16)
            home(k).start()

    def final(i):
        return remote(sq.at[0], sq.at[i], q_s.at[i], q_r.at[i], planes[i - 1])

    across(0).wait_recv()
    combined = acc[0, c] + drecv[0].astype(F32)
    for k in range(1, chunks):
        home(k).wait_recv()
        combined = combined + zrecv[k].astype(F32)
    sq[0] = jnp.broadcast_to(jnp.sum(combined * combined, axis=1, keepdims=True), (rows, lanes))
    for i in range(1, 4):
        final(i).start()
    acc[0, c] = combined
    for i in range(1, 4):
        final(i).wait_recv()
    total = jnp.sum(sq[...], axis=0)
    out_scale = jnp.concatenate([lax.rsqrt(total / D + epsilon)] * (width // lanes), axis=1)
    o_ref[...] = (acc[0, c] * out_scale * go_ref[...]).astype(BF16)

    forward(0).wait_send()
    across(0).wait_send()
    for i in range(1, 4):
        gather(i).wait_send()
        forward(i).wait_send()
        squares(i).wait_send()
        across(i).wait_send()
        home(i).wait_send()
        final(i).wait_send()
    for k in range(chunks):
        for e in range(2):
            for phase in (phase1, phase2, phase3, phase4):
                phase(k, e).wait_send()


def dense_on_device(
    tokens, expert_ids, route_weights, gain_in, gain_out, gate_weights, up_weights, down_weights
):
    rows, width = tokens.shape
    ff = gate_weights.shape[2]
    half, quarter, lanes = ff // 2, ff // 4, 128
    chunks = lax.axis_size("ep") // 2
    both = 2 * rows
    vmem = pl.BlockSpec(memory_space=pltpu.VMEM)
    hbm = pl.BlockSpec(memory_space=pltpu.HBM)
    dma = pltpu.SemaphoreType.DMA
    one, two = dma((chunks,)), dma((chunks, 2))
    return pl.pallas_call(
        dense_kernel,
        out_shape=jax.ShapeDtypeStruct((rows, width), BF16),
        in_specs=[vmem] * 5 + [hbm] * 3,
        out_specs=vmem,
        scratch_shapes=[
            pltpu.VMEM((2, 2, width, half), BF16),
            pltpu.VMEM((2, 2, 2, width, quarter), BF16),
            pltpu.VMEM((2, ff, width), BF16),
            pltpu.VMEM((chunks, 2, rows, width + lanes), BF16),
            pltpu.VMEM((chunks, both, width), BF16),
            pltpu.VMEM((chunks, both, lanes), F32),
            pltpu.VMEM((4, 8, chunks * both), F32),
            pltpu.VMEM((chunks, both, lanes), F32),
            pltpu.VMEM((chunks, 2, both, lanes), F32),
            pltpu.VMEM((chunks, 2, 2, 2, both, quarter), BF16),
            pltpu.VMEM((chunks, 2, 2, 2, both, quarter), BF16),
            pltpu.VMEM((chunks, 2, 2, both, quarter), BF16),
            pltpu.VMEM((chunks, 2, 2, both, quarter), BF16),
            pltpu.VMEM((chunks, 2, 2, both, quarter), F32),
            pltpu.VMEM((chunks, 2, 4, both, quarter), BF16),
            pltpu.VMEM((chunks, 2, rows, width), F32),
            pltpu.VMEM((chunks, rows, width), BF16),
            pltpu.VMEM((chunks, rows, width), BF16),
            pltpu.VMEM((chunks, rows, width), BF16),
            pltpu.VMEM((chunks, rows, width), BF16),
            pltpu.VMEM((4, rows, lanes), F32),
            dma((14,)),
        ]
        + [one] * 6
        + [two] * 8
        + [one] * 6,
        compiler_params=pltpu.CompilerParams(
            collective_id=0, has_side_effects=True, vmem_limit_bytes=60 * 1024 * 1024
        ),
    )(
        tokens, expert_ids, route_weights, gain_in[None, :], gain_out[None, :],
        gate_weights, up_weights, down_weights,
    )


def device_program(*args):
    tokens, expert_ids = args[:2]
    local_experts = args[5].shape[0]
    all_experts = local_experts * lax.axis_size("ep")
    capacity = max(2, 2 * tokens.shape[0] * expert_ids.shape[1] // all_experts)
    dense = capacity >= tokens.shape[0] and all_experts <= 64
    if dense and (local_experts, lax.axis_size("ep"), lax.axis_size("tp")) == (2, 8, 4):
        return dense_on_device(*args)
    return on_device(*args)


def solution(mesh):
    placed = (
        P("ep", "tp"),
        P("ep", None),
        P("ep", None),
        P("tp"),
        P("tp"),
        P("ep", "tp", None),
        P("ep", "tp", None),
        P("ep", None, "tp"),
    )
    return jax.shard_map(
        device_program, mesh=mesh, in_specs=placed, out_specs=P("ep", "tp"), check_vma=False
    )
```

```python
import jax
import jax.numpy as jnp
from jax import lax
from jax.experimental import pallas as pl
from jax.experimental.pallas import tpu as pltpu
from jax.sharding import PartitionSpec as P

D = 4096


epsilon = 1e-06


def expert_apply(incoming, gate_weights, up_weights, down_weights):
    gate_part = jnp.einsum(
        "secd,edf->secf", incoming, gate_weights, preferred_element_type=jnp.float32
    ).astype(jnp.bfloat16)
    up_part = jnp.einsum(
        "secd,edf->secf", incoming, up_weights, preferred_element_type=jnp.float32
    ).astype(jnp.bfloat16)
    gate_sum, up_sum = (
        lax.psum(gate_part, "tp").astype(jnp.float32),
        lax.psum(up_part, "tp").astype(jnp.float32),
    )
    hidden = (jax.nn.silu(gate_sum) * up_sum).astype(jnp.bfloat16)
    total = jnp.einsum("secf,efd->secd", hidden, down_weights, preferred_element_type=jnp.float32)
    return total.astype(jnp.bfloat16)


def on_device(
    tokens, expert_ids, route_weights, gain_in, gain_out, gate_weights, up_weights, down_weights
):
    tok_count, local_width = tokens.shape
    top_count = expert_ids.shape[1]
    local_experts = gate_weights.shape[0]
    ep_count = lax.axis_size("ep")
    all_experts = local_experts * ep_count
    capacity = max(2, 2 * tok_count * top_count // all_experts)
    widened = tokens.astype(jnp.float32)
    squares = lax.psum(jnp.sum(widened * widened, axis=1), "tp")
    normed = (widened * lax.rsqrt(squares / D + epsilon)[:, None] * gain_in[None, :]).astype(
        jnp.bfloat16
    )
    pair_ids = expert_ids.reshape(-1)
    expert_hot = (pair_ids[:, None] == jnp.arange(all_experts, dtype=jnp.int32)[None, :]).astype(
        jnp.int32
    )
    slot_rank = jnp.sum((jnp.cumsum(expert_hot, axis=0) - 1) * expert_hot, axis=1)
    slot_ids = pair_ids * capacity + slot_rank
    slot_hot = (
        slot_ids[:, None] == jnp.arange(all_experts * capacity, dtype=jnp.int32)[None, :]
    ).astype(jnp.float32)
    pair_rows = jnp.repeat(normed, top_count, axis=0)
    outgoing = jnp.einsum(
        "ps,pd->sd", slot_hot.astype(jnp.bfloat16), pair_rows, preferred_element_type=jnp.float32
    ).astype(jnp.bfloat16)
    incoming = lax.all_to_all(
        outgoing.reshape(ep_count, local_experts, capacity, local_width),
        "ep",
        split_axis=0,
        concat_axis=0,
        tiled=True,
    )
    results = expert_apply(incoming, gate_weights, up_weights, down_weights)
    returned = lax.all_to_all(results, "ep", split_axis=0, concat_axis=0, tiled=True)
    weighting = jnp.sum(
        (slot_hot * route_weights.reshape(-1)[:, None]).reshape(tok_count, top_count, -1), axis=1
    )
    combined = jnp.dot(
        weighting,
        returned.reshape(-1, local_width).astype(jnp.float32),
        precision=lax.Precision.HIGHEST,
    )
    out_squares = lax.psum(jnp.sum(combined * combined, axis=1), "tp")
    return (combined * lax.rsqrt(out_squares / D + epsilon)[:, None] * gain_out[None, :]).astype(
        jnp.bfloat16
    )


MESH = pl.DeviceIdType.MESH
BF16, F32 = jnp.bfloat16, jnp.float32


def remote(src, dst, send_sem, recv_sem, target):
    return pltpu.make_async_remote_copy(
        src_ref=src,
        dst_ref=dst,
        send_sem=send_sem,
        recv_sem=recv_sem,
        device_id=target,
        device_id_type=MESH,
    )


def chip_at(z, k):
    low = lax.rem(lax.rem(z, 2) + lax.rem(k, 2), 2)
    high = lax.rem(z // 2 + k // 2, 2)
    return high * 2 + low


def dense_kernel(
    x_ref, ids_ref, rw_ref, gi_ref, go_ref, gate_hbm, up_hbm, down_hbm, o_ref,
    w0, w1, dw, xg, xs, ssb, sst, scale, wr, sbuf, r1, s2, r2, keep, hid,
    acc, dsend, drecv, zsend, zrecv, sq,
    wsem, ag_s, ag_r, fw_s, fw_r, ss_s, ss_r, p1_s, p1_r, p2_s, p2_r, p3_s, p3_r,
    p4_s, p4_r, d_s, d_r, z_s, z_r, q_s, q_r,
):
    rows, width = x_ref.shape
    chunks = xg.shape[0]
    half = w0.shape[3]
    quarter = half // 2
    lanes = ssb.shape[2]
    ep, tp = lax.axis_index("ep"), lax.axis_index("tp")
    z, c = ep // 2, lax.rem(ep, 2)
    y, x = tp // 2, lax.rem(tp, 2)
    xn, yn, dn = y * 2 + 1 - x, (1 - y) * 2 + x, (1 - y) * 2 + 1 - x
    other = z * 2 + 1 - c
    first = ((ep, xn), (ep, yn))
    second = ((ep, yn), (ep, xn))
    big, small = (x, y), (y, x)
    planes = ((ep, xn), (ep, yn), (ep, dn))

    barrier = pltpu.get_barrier_semaphore()
    greet = [(other, tp)] + [(chip_at(z, k) * 2 + c, tp) for k in range(1, chunks)] + list(planes)
    for target in greet:
        pl.semaphore_signal(barrier, inc=1, device_id=target, device_id_type=MESH)

    mats = (gate_hbm, up_hbm)
    load0, load1, load2 = [], [], []
    for e in range(2):
        for m in range(2):
            off = pl.multiple_of((1 - big[e]) * half, quarter)
            load0.append(pltpu.make_async_copy(
                mats[m].at[e, :, pl.ds(off, half)], w0.at[e, m], wsem.at[e * 2 + m]))
            for s in range(2):
                q = small[e] if s else 1 - small[e]
                off = pl.multiple_of(big[e] * half + q * quarter, quarter)
                load1.append(pltpu.make_async_copy(
                    mats[m].at[e, :, pl.ds(off, quarter)], w1.at[e, m, s],
                    wsem.at[4 + e * 4 + m * 2 + s]))
        load2.append(pltpu.make_async_copy(down_hbm.at[e], dw.at[e], wsem.at[12 + e]))
    for load in load0:
        load.start()

    lane = lax.broadcasted_iota(jnp.int32, (rows, lanes), 1)
    place = lax.broadcasted_iota(jnp.int32, (lanes, rows), 0)
    ids, rw = ids_ref[...], rw_ref[...]
    route = jnp.zeros((lanes, rows), F32)
    for k in range(ids.shape[0]):
        hit = (ids[k : k + 1] == place) | (ids[k : k + 1] == place - lanes // 2)
        route = route + jnp.where(hit, rw[k : k + 1], 0.0)
    route = jnp.transpose(route)
    high = route.astype(BF16)
    low = (route - high.astype(F32)).astype(BF16)
    xg[0, c, :, :width] = x_ref[...]
    xg[0, c, :, width:] = jnp.where(
        lane < lanes // 2, high.astype(F32), low.astype(F32)
    ).astype(BF16)

    pl.semaphore_wait(barrier, len(greet))

    def gather(k):
        return remote(xg.at[0, c], xg.at[k, c], ag_s.at[k], ag_r.at[k], (chip_at(z, k) * 2 + c, tp))

    def forward(k):
        return remote(xg.at[k, c], xg.at[k, c], fw_s.at[k], fw_r.at[k], (other, tp))

    forward(0).start()
    for k in range(1, chunks):
        gather(k).start()
    for load in load1 + load2:
        load.start()

    gain = gi_ref[...]

    def phase1(k, e):
        return remote(sbuf.at[k, e], r1.at[k, e], p1_s.at[k, e], p1_r.at[k, e], first[e])

    def phase2(k, e):
        return remote(s2.at[k, e], r2.at[k, e], p2_s.at[k, e], p2_r.at[k, e], second[e])

    def phase3(k, e):
        block = hid.at[k, e, big[e] * 2 + small[e]]
        return remote(block, block, p3_s.at[k, e], p3_r.at[k, e], second[e])

    def phase4(k, e):
        block = hid.at[k, e, pl.ds(big[e] * 2, 2)]
        return remote(block, block, p4_s.at[k, e], p4_r.at[k, e], first[e])

    def across(k):
        return remote(dsend.at[k], drecv.at[k], d_s.at[k], d_r.at[k], (other, tp))

    def home(k):
        return remote(zsend.at[k], zrecv.at[k], z_s.at[k], z_r.at[k], (chip_at(z, k) * 2 + c, tp))

    @pl.loop(0, chunks)
    def _(k):
        @pl.when(k > 0)
        def _():
            gather(k).wait_recv()
            forward(k).start()

        forward(k).wait_recv()
        for j in range(2):
            at = pl.ds(j * rows, rows)
            xf = xg[k, j, :, :width].astype(F32)
            ssb[k, at, :] = jnp.broadcast_to(
                jnp.sum(xf * xf, axis=1, keepdims=True), (rows, lanes))
            xs[k, at, :] = (xf * gain).astype(BF16)
            r = xg[k, j, :, width:].astype(F32)
            for e in range(2):
                mine = ep * 2 + e
                hit = (lane == mine) | (lane == mine + lanes // 2)
                wr[k, e, at, :] = jnp.broadcast_to(
                    jnp.sum(jnp.where(hit, r, 0.0), axis=1, keepdims=True), (rows, lanes))
        for e in range(2):
            @pl.when(k == 0)
            def _():
                for load in load0[2 * e : 2 * e + 2]:
                    load.wait()

            for m in range(2):
                p = jnp.dot(xs[k], w0[e, m], preferred_element_type=F32).astype(BF16)
                sbuf[k, e, m, 0] = p[:, :quarter]
                sbuf[k, e, m, 1] = p[:, quarter:]
            phase1(k, e).start()

    def squares(i):
        return remote(sst.at[0], sst.at[i], ss_s.at[i], ss_r.at[i], planes[i - 1])

    sst[0] = jnp.transpose(ssb[...].reshape(chunks * 2 * rows, lanes))[:8]
    for i in range(1, 4):
        squares(i).start()
    for load in load1:
        load.wait()

    def order(i):
        return lax.rem(i + 1, chunks)

    @pl.loop(0, chunks)
    def _(i):
        k = order(i)
        for e in range(2):
            phase1(k, e).wait_recv()
            for m in range(2):
                p = jnp.dot(xs[k], w1[e, m, 0], preferred_element_type=F32)
                s2[k, e, m] = (p + r1[k, e, m, 1 - small[e]].astype(F32)).astype(BF16)
            phase2(k, e).start()
            for m in range(2):
                p = jnp.dot(xs[k], w1[e, m, 1], preferred_element_type=F32)
                keep[k, e, m] = p + r1[k, e, m, small[e]].astype(F32)

    for i in range(1, 4):
        squares(i).wait_recv()
    total = jnp.sum(sst[...], axis=0)
    total = jnp.transpose(jnp.concatenate([total] * (lanes // 8), axis=0))
    scale[...] = lax.rsqrt(total / D + epsilon).reshape(scale.shape)
    for load in load2:
        load.wait()

    @pl.loop(0, chunks + 3)
    def _(i):
        @pl.when(i < chunks)
        def _():
            k = order(i)
            s = jnp.concatenate([scale[k]] * (quarter // lanes), axis=1)
            for e in range(2):
                phase2(k, e).wait_recv()
                g = (keep[k, e, 0] + r2[k, e, 0].astype(F32)) * s
                u = (keep[k, e, 1] + r2[k, e, 1].astype(F32)) * s
                w = jnp.concatenate([wr[k, e]] * (quarter // lanes), axis=1)
                h = g / (1.0 + jnp.exp(-g)) * u * w
                hid[k, e, big[e] * 2 + small[e]] = h.astype(BF16)
                phase3(k, e).start()

        @pl.when((i >= 1) & (i < chunks + 1))
        def _():
            k = order(i - 1)
            for e in range(2):
                phase3(k, e).wait_recv()
                phase4(k, e).start()

        @pl.when((i >= 2) & (i < chunks + 2))
        def _():
            k = order(i - 2)
            for e in range(2):
                phase4(k, e).wait_recv()
            hcat = jnp.concatenate([hid[k, e, q] for e in range(2) for q in range(4)], axis=1)
            for n in range(0, width, half):
                cols = pl.ds(n, half)
                down = jnp.concatenate([dw[0, :, cols], dw[1, :, cols]], axis=0)
                p = jnp.dot(hcat, down, preferred_element_type=F32)
                acc[k, 0, :, cols] = p[:rows]
                acc[k, 1, :, cols] = p[rows:]
            dsend[k] = acc[k, 1 - c].astype(BF16)
            across(k).start()

        @pl.when((i >= 3) & (i < chunks + 2))
        def _():
            k = order(i - 3)
            across(k).wait_recv()
            zsend[k] = (acc[k, c] + drecv[k].astype(F32)).astype(BF16)
            home(k).start()

    def final(i):
        return remote(sq.at[0], sq.at[i], q_s.at[i], q_r.at[i], planes[i - 1])

    across(0).wait_recv()
    combined = acc[0, c] + drecv[0].astype(F32)
    for k in range(1, chunks):
        home(k).wait_recv()
        combined = combined + zrecv[k].astype(F32)
    sq[0] = jnp.broadcast_to(jnp.sum(combined * combined, axis=1, keepdims=True), (rows, lanes))
    for i in range(1, 4):
        final(i).start()
    acc[0, c] = combined
    for i in range(1, 4):
        final(i).wait_recv()
    total = jnp.sum(sq[...], axis=0)
    out_scale = jnp.concatenate([lax.rsqrt(total / D + epsilon)] * (width // lanes), axis=1)
    o_ref[...] = (acc[0, c] * out_scale * go_ref[...]).astype(BF16)

    forward(0).wait_send()
    across(0).wait_send()
    for i in range(1, 4):
        gather(i).wait_send()
        forward(i).wait_send()
        squares(i).wait_send()
        across(i).wait_send()
        home(i).wait_send()
        final(i).wait_send()
    for k in range(chunks):
        for e in range(2):
            for phase in (phase1, phase2, phase3, phase4):
                phase(k, e).wait_send()


def dense_on_device(
    tokens, expert_ids, route_weights, gain_in, gain_out, gate_weights, up_weights, down_weights
):
    rows, width = tokens.shape
    ff = gate_weights.shape[2]
    half, quarter, lanes = ff // 2, ff // 4, 128
    chunks = lax.axis_size("ep") // 2
    both = 2 * rows
    vmem = pl.BlockSpec(memory_space=pltpu.VMEM)
    hbm = pl.BlockSpec(memory_space=pltpu.HBM)
    dma = pltpu.SemaphoreType.DMA
    one, two = dma((chunks,)), dma((chunks, 2))
    return pl.pallas_call(
        dense_kernel,
        out_shape=jax.ShapeDtypeStruct((rows, width), BF16),
        in_specs=[vmem] * 5 + [hbm] * 3,
        out_specs=vmem,
        scratch_shapes=[
            pltpu.VMEM((2, 2, width, half), BF16),
            pltpu.VMEM((2, 2, 2, width, quarter), BF16),
            pltpu.VMEM((2, ff, width), BF16),
            pltpu.VMEM((chunks, 2, rows, width + lanes), BF16),
            pltpu.VMEM((chunks, both, width), BF16),
            pltpu.VMEM((chunks, both, lanes), F32),
            pltpu.VMEM((4, 8, chunks * both), F32),
            pltpu.VMEM((chunks, both, lanes), F32),
            pltpu.VMEM((chunks, 2, both, lanes), F32),
            pltpu.VMEM((chunks, 2, 2, 2, both, quarter), BF16),
            pltpu.VMEM((chunks, 2, 2, 2, both, quarter), BF16),
            pltpu.VMEM((chunks, 2, 2, both, quarter), BF16),
            pltpu.VMEM((chunks, 2, 2, both, quarter), BF16),
            pltpu.VMEM((chunks, 2, 2, both, quarter), F32),
            pltpu.VMEM((chunks, 2, 4, both, quarter), BF16),
            pltpu.VMEM((chunks, 2, rows, width), F32),
            pltpu.VMEM((chunks, rows, width), BF16),
            pltpu.VMEM((chunks, rows, width), BF16),
            pltpu.VMEM((chunks, rows, width), BF16),
            pltpu.VMEM((chunks, rows, width), BF16),
            pltpu.VMEM((4, rows, lanes), F32),
            dma((14,)),
        ]
        + [one] * 6
        + [two] * 8
        + [one] * 6,
        compiler_params=pltpu.CompilerParams(
            collective_id=0, has_side_effects=True, vmem_limit_bytes=60 * 1024 * 1024
        ),
    )(
        tokens, expert_ids.T, route_weights.T, gain_in[None, :], gain_out[None, :],
        gate_weights, up_weights, down_weights,
    )


def device_program(*args):
    tokens, expert_ids = args[:2]
    local_experts = args[5].shape[0]
    all_experts = local_experts * lax.axis_size("ep")
    capacity = max(2, 2 * tokens.shape[0] * expert_ids.shape[1] // all_experts)
    dense = capacity >= tokens.shape[0] and all_experts <= 64
    if dense and (local_experts, lax.axis_size("ep"), lax.axis_size("tp")) == (2, 8, 4):
        return dense_on_device(*args)
    return on_device(*args)


def solution(mesh):
    placed = (
        P("ep", "tp"),
        P("ep", None),
        P("ep", None),
        P("tp"),
        P("tp"),
        P("ep", "tp", None),
        P("ep", "tp", None),
        P("ep", None, "tp"),
    )
    return jax.shard_map(
        device_program, mesh=mesh, in_specs=placed, out_specs=P("ep", "tp"), check_vma=False
    )
```

```python
import jax
import jax.numpy as jnp
from jax import lax
from jax.experimental import pallas as pl
from jax.experimental.pallas import tpu as pltpu
from jax.sharding import PartitionSpec as P

D = 4096


epsilon = 1e-06


def expert_apply(incoming, gate_weights, up_weights, down_weights):
    gate_part = jnp.einsum(
        "secd,edf->secf", incoming, gate_weights, preferred_element_type=jnp.float32
    ).astype(jnp.bfloat16)
    up_part = jnp.einsum(
        "secd,edf->secf", incoming, up_weights, preferred_element_type=jnp.float32
    ).astype(jnp.bfloat16)
    gate_sum, up_sum = (
        lax.psum(gate_part, "tp").astype(jnp.float32),
        lax.psum(up_part, "tp").astype(jnp.float32),
    )
    hidden = (jax.nn.silu(gate_sum) * up_sum).astype(jnp.bfloat16)
    total = jnp.einsum("secf,efd->secd", hidden, down_weights, preferred_element_type=jnp.float32)
    return total.astype(jnp.bfloat16)


def on_device(
    tokens, expert_ids, route_weights, gain_in, gain_out, gate_weights, up_weights, down_weights
):
    tok_count, local_width = tokens.shape
    top_count = expert_ids.shape[1]
    local_experts = gate_weights.shape[0]
    ep_count = lax.axis_size("ep")
    all_experts = local_experts * ep_count
    capacity = max(2, 2 * tok_count * top_count // all_experts)
    widened = tokens.astype(jnp.float32)
    squares = lax.psum(jnp.sum(widened * widened, axis=1), "tp")
    normed = (widened * lax.rsqrt(squares / D + epsilon)[:, None] * gain_in[None, :]).astype(
        jnp.bfloat16
    )
    pair_ids = expert_ids.reshape(-1)
    expert_hot = (pair_ids[:, None] == jnp.arange(all_experts, dtype=jnp.int32)[None, :]).astype(
        jnp.int32
    )
    slot_rank = jnp.sum((jnp.cumsum(expert_hot, axis=0) - 1) * expert_hot, axis=1)
    slot_ids = pair_ids * capacity + slot_rank
    slot_hot = (
        slot_ids[:, None] == jnp.arange(all_experts * capacity, dtype=jnp.int32)[None, :]
    ).astype(jnp.float32)
    pair_rows = jnp.repeat(normed, top_count, axis=0)
    outgoing = jnp.einsum(
        "ps,pd->sd", slot_hot.astype(jnp.bfloat16), pair_rows, preferred_element_type=jnp.float32
    ).astype(jnp.bfloat16)
    incoming = lax.all_to_all(
        outgoing.reshape(ep_count, local_experts, capacity, local_width),
        "ep",
        split_axis=0,
        concat_axis=0,
        tiled=True,
    )
    results = expert_apply(incoming, gate_weights, up_weights, down_weights)
    returned = lax.all_to_all(results, "ep", split_axis=0, concat_axis=0, tiled=True)
    weighting = jnp.sum(
        (slot_hot * route_weights.reshape(-1)[:, None]).reshape(tok_count, top_count, -1), axis=1
    )
    combined = jnp.dot(
        weighting,
        returned.reshape(-1, local_width).astype(jnp.float32),
        precision=lax.Precision.HIGHEST,
    )
    out_squares = lax.psum(jnp.sum(combined * combined, axis=1), "tp")
    return (combined * lax.rsqrt(out_squares / D + epsilon)[:, None] * gain_out[None, :]).astype(
        jnp.bfloat16
    )


MESH = pl.DeviceIdType.MESH
BF16, F32 = jnp.bfloat16, jnp.float32


def remote(src, dst, send_sem, recv_sem, target):
    return pltpu.make_async_remote_copy(
        src_ref=src,
        dst_ref=dst,
        send_sem=send_sem,
        recv_sem=recv_sem,
        device_id=target,
        device_id_type=MESH,
    )


def chip_at(z, k):
    low = lax.rem(lax.rem(z, 2) + lax.rem(k, 2), 2)
    high = lax.rem(z // 2 + k // 2, 2)
    return high * 2 + low


def dense_kernel(
    x_ref, ids_ref, rw_ref, gi_ref, go_ref, gate_hbm, up_hbm, down_hbm, o_ref,
    w0, w1, dw, xg, xs, ssb, sst, scale, wr, sbuf, r1, s2, r2, own, hid,
    acc, dsend, drecv, zsend, zrecv, sq,
    wsem, ag_s, ag_r, fw_s, fw_r, ss_s, ss_r, p1_s, p1_r, p2_s, p2_r, p3_s, p3_r,
    p4_s, p4_r, d_s, d_r, z_s, z_r, q_s, q_r,
):
    rows, width = x_ref.shape
    chunks = xg.shape[0]
    half = w0.shape[3]
    quarter = half // 2
    lanes = ssb.shape[2]
    ep, tp = lax.axis_index("ep"), lax.axis_index("tp")
    z, c = ep // 2, lax.rem(ep, 2)
    y, x = tp // 2, lax.rem(tp, 2)
    xn, yn, dn = y * 2 + 1 - x, (1 - y) * 2 + x, (1 - y) * 2 + 1 - x
    other = z * 2 + 1 - c
    first = ((ep, xn), (ep, yn))
    second = ((ep, yn), (ep, xn))
    big, small = (x, y), (y, x)
    planes = ((ep, xn), (ep, yn), (ep, dn))

    barrier = pltpu.get_barrier_semaphore()
    greet = [(other, tp)] + [(chip_at(z, k) * 2 + c, tp) for k in range(1, chunks)] + list(planes)
    for target in greet:
        pl.semaphore_signal(barrier, inc=1, device_id=target, device_id_type=MESH)

    mats = (gate_hbm, up_hbm)
    load0, load1, load2 = [], [], []
    for e in range(2):
        for m in range(2):
            off = pl.multiple_of((1 - big[e]) * half, quarter)
            load0.append(pltpu.make_async_copy(
                mats[m].at[e, :, pl.ds(off, half)], w0.at[e, m], wsem.at[e * 2 + m]))
            for s in range(2):
                q = small[e] if s else 1 - small[e]
                off = pl.multiple_of(big[e] * half + q * quarter, quarter)
                load1.append(pltpu.make_async_copy(
                    mats[m].at[e, :, pl.ds(off, quarter)], w1.at[e, m, s],
                    wsem.at[4 + e * 4 + m * 2 + s]))
        load2.append(pltpu.make_async_copy(down_hbm.at[e], dw.at[e], wsem.at[12 + e]))
    for load in load0:
        load.start()

    lane = lax.broadcasted_iota(jnp.int32, (rows, lanes), 1)
    place = lax.broadcasted_iota(jnp.int32, (lanes, rows), 0)
    ids, rw = ids_ref[...], rw_ref[...]
    route = jnp.zeros((lanes, rows), F32)
    for k in range(ids.shape[0]):
        hit = (ids[k : k + 1] == place) | (ids[k : k + 1] == place - lanes // 2)
        route = route + jnp.where(hit, rw[k : k + 1], 0.0)
    route = jnp.transpose(route)
    high = route.astype(BF16)
    low = (route - high.astype(F32)).astype(BF16)
    xg[0, c, :, :width] = x_ref[...]
    xg[0, c, :, width:] = jnp.where(
        lane < lanes // 2, high.astype(F32), low.astype(F32)
    ).astype(BF16)

    pl.semaphore_wait(barrier, len(greet))

    def gather(k):
        return remote(xg.at[0, c], xg.at[k, c], ag_s.at[k], ag_r.at[k], (chip_at(z, k) * 2 + c, tp))

    def forward(k):
        return remote(xg.at[k, c], xg.at[k, c], fw_s.at[k], fw_r.at[k], (other, tp))

    forward(0).start()
    for k in range(1, chunks):
        gather(k).start()
    for load in load1 + load2:
        load.start()

    gain = gi_ref[...]

    def phase1(k, e):
        return remote(sbuf.at[k, e], r1.at[k, e], p1_s.at[k, e], p1_r.at[k, e], first[e])

    def phase2(k, e):
        return remote(s2.at[k, e], r2.at[k, e], p2_s.at[k, e], p2_r.at[k, e], second[e])

    def phase3(k, e):
        block = hid.at[k, e, big[e] * 2 + small[e]]
        return remote(block, block, p3_s.at[k, e], p3_r.at[k, e], second[e])

    def phase4(k, e):
        block = hid.at[k, e, pl.ds(big[e] * 2, 2)]
        return remote(block, block, p4_s.at[k, e], p4_r.at[k, e], first[e])

    def across(k):
        return remote(dsend.at[k], drecv.at[k], d_s.at[k], d_r.at[k], (other, tp))

    def home(k):
        return remote(zsend.at[k], zrecv.at[k], z_s.at[k], z_r.at[k], (chip_at(z, k) * 2 + c, tp))

    def own_products(k):
        for e in range(2):
            for s in range(2):
                for m in range(2):
                    own[k, e, m, s] = jnp.dot(xs[k], w1[e, m, s], preferred_element_type=F32)

    @pl.loop(0, chunks)
    def _(k):
        @pl.when(k > 0)
        def _():
            gather(k).wait_recv()
            forward(k).start()

        forward(k).wait_recv()
        for j in range(2):
            at = pl.ds(j * rows, rows)
            xf = xg[k, j, :, :width].astype(F32)
            ssb[k, at, :] = jnp.broadcast_to(
                jnp.sum(xf * xf, axis=1, keepdims=True), (rows, lanes))
            xs[k, at, :] = (xf * gain).astype(BF16)
            r = xg[k, j, :, width:].astype(F32)
            for e in range(2):
                mine = ep * 2 + e
                hit = (lane == mine) | (lane == mine + lanes // 2)
                wr[k, e, at, :] = jnp.broadcast_to(
                    jnp.sum(jnp.where(hit, r, 0.0), axis=1, keepdims=True), (rows, lanes))
        for e in range(2):
            @pl.when(k == 0)
            def _():
                for load in load0[2 * e : 2 * e + 2]:
                    load.wait()

            for m in range(2):
                p = jnp.dot(xs[k], w0[e, m], preferred_element_type=F32).astype(BF16)
                sbuf[k, e, m, 0] = p[:, :quarter]
                sbuf[k, e, m, 1] = p[:, quarter:]
            phase1(k, e).start()

        @pl.when(k > 0)
        def _():
            @pl.when(k == 1)
            def _():
                for load in load1:
                    load.wait()

            own_products(k - 1)

    def squares(i):
        return remote(sst.at[0], sst.at[i], ss_s.at[i], ss_r.at[i], planes[i - 1])

    sst[0] = jnp.transpose(ssb[...].reshape(chunks * 2 * rows, lanes))[:8]
    for i in range(1, 4):
        squares(i).start()
    own_products(chunks - 1)

    def order(i):
        return lax.rem(i + 1, chunks)

    @pl.loop(0, chunks)
    def _(i):
        k = order(i)
        for e in range(2):
            phase1(k, e).wait_recv()
            for m in range(2):
                away = r1[k, e, m, 1 - small[e]].astype(F32)
                s2[k, e, m] = (own[k, e, m, 0] + away).astype(BF16)
            phase2(k, e).start()

    for i in range(1, 4):
        squares(i).wait_recv()
    total = jnp.sum(sst[...], axis=0)
    total = jnp.transpose(jnp.concatenate([total] * (lanes // 8), axis=0))
    scale[...] = lax.rsqrt(total / D + epsilon).reshape(scale.shape)

    @pl.loop(0, chunks)
    def _(i):
        k = order(i)
        s = jnp.concatenate([scale[k]] * (quarter // lanes), axis=1)
        for e in range(2):
            w = jnp.concatenate([wr[k, e]] * (quarter // lanes), axis=1)
            mine = [own[k, e, m, 1] + r1[k, e, m, small[e]].astype(F32) for m in range(2)]
            phase2(k, e).wait_recv()
            g = (mine[0] + r2[k, e, 0].astype(F32)) * s
            u = (mine[1] + r2[k, e, 1].astype(F32)) * s
            h = g / (1.0 + jnp.exp(-g)) * u * w
            hid[k, e, big[e] * 2 + small[e]] = h.astype(BF16)
            phase3(k, e).start()

    for load in load2:
        load.wait()

    @pl.loop(0, chunks)
    def _(i):
        k = order(i)
        for e in range(2):
            phase3(k, e).wait_recv()
            phase4(k, e).start()

    @pl.loop(0, chunks)
    def _(i):
        k = order(i)
        for e in range(2):
            phase4(k, e).wait_recv()
        hcat = jnp.concatenate([hid[k, e, q] for e in range(2) for q in range(4)], axis=1)
        for n in range(0, width, half):
            cols = pl.ds(n, half)
            down = jnp.concatenate([dw[0, :, cols], dw[1, :, cols]], axis=0)
            p = jnp.dot(hcat, down, preferred_element_type=F32)
            acc[k, 0, :, cols] = p[:rows]
            acc[k, 1, :, cols] = p[rows:]
        dsend[k] = acc[k, 1 - c].astype(BF16)
        across(k).start()

        @pl.when(i >= 1)
        def _():
            b = order(i - 1)
            across(b).wait_recv()
            zsend[b] = (acc[b, c] + drecv[b].astype(F32)).astype(BF16)
            home(b).start()

    def final(i):
        return remote(sq.at[0], sq.at[i], q_s.at[i], q_r.at[i], planes[i - 1])

    combined = acc[0, c]
    for k in range(1, chunks):
        home(k).wait_recv()
        combined = combined + zrecv[k].astype(F32)
    across(0).wait_recv()
    combined = combined + drecv[0].astype(F32)
    sq[0] = jnp.broadcast_to(jnp.sum(combined * combined, axis=1, keepdims=True), (rows, lanes))
    for i in range(1, 4):
        final(i).start()
    acc[0, c] = combined
    for i in range(1, 4):
        final(i).wait_recv()
    total = jnp.sum(sq[...], axis=0)
    out_scale = jnp.concatenate([lax.rsqrt(total / D + epsilon)] * (width // lanes), axis=1)
    o_ref[...] = (acc[0, c] * out_scale * go_ref[...]).astype(BF16)

    forward(0).wait_send()
    across(0).wait_send()
    for i in range(1, 4):
        gather(i).wait_send()
        forward(i).wait_send()
        squares(i).wait_send()
        across(i).wait_send()
        home(i).wait_send()
        final(i).wait_send()
    for k in range(chunks):
        for e in range(2):
            for phase in (phase1, phase2, phase3, phase4):
                phase(k, e).wait_send()


def dense_on_device(
    tokens, expert_ids, route_weights, gain_in, gain_out, gate_weights, up_weights, down_weights
):
    rows, width = tokens.shape
    ff = gate_weights.shape[2]
    half, quarter, lanes = ff // 2, ff // 4, 128
    chunks = lax.axis_size("ep") // 2
    both = 2 * rows
    vmem = pl.BlockSpec(memory_space=pltpu.VMEM)
    hbm = pl.BlockSpec(memory_space=pltpu.HBM)
    dma = pltpu.SemaphoreType.DMA
    one, two = dma((chunks,)), dma((chunks, 2))
    return pl.pallas_call(
        dense_kernel,
        out_shape=jax.ShapeDtypeStruct((rows, width), BF16),
        in_specs=[vmem] * 5 + [hbm] * 3,
        out_specs=vmem,
        scratch_shapes=[
            pltpu.VMEM((2, 2, width, half), BF16),
            pltpu.VMEM((2, 2, 2, width, quarter), BF16),
            pltpu.VMEM((2, ff, width), BF16),
            pltpu.VMEM((chunks, 2, rows, width + lanes), BF16),
            pltpu.VMEM((chunks, both, width), BF16),
            pltpu.VMEM((chunks, both, lanes), F32),
            pltpu.VMEM((4, 8, chunks * both), F32),
            pltpu.VMEM((chunks, both, lanes), F32),
            pltpu.VMEM((chunks, 2, both, lanes), F32),
            pltpu.VMEM((chunks, 2, 2, 2, both, quarter), BF16),
            pltpu.VMEM((chunks, 2, 2, 2, both, quarter), BF16),
            pltpu.VMEM((chunks, 2, 2, both, quarter), BF16),
            pltpu.VMEM((chunks, 2, 2, both, quarter), BF16),
            pltpu.VMEM((chunks, 2, 2, 2, both, quarter), F32),
            pltpu.VMEM((chunks, 2, 4, both, quarter), BF16),
            pltpu.VMEM((chunks, 2, rows, width), F32),
            pltpu.VMEM((chunks, rows, width), BF16),
            pltpu.VMEM((chunks, rows, width), BF16),
            pltpu.VMEM((chunks, rows, width), BF16),
            pltpu.VMEM((chunks, rows, width), BF16),
            pltpu.VMEM((4, rows, lanes), F32),
            dma((14,)),
        ]
        + [one] * 6
        + [two] * 8
        + [one] * 6,
        compiler_params=pltpu.CompilerParams(
            collective_id=0, has_side_effects=True, vmem_limit_bytes=60 * 1024 * 1024
        ),
    )(
        tokens, expert_ids.T, route_weights.T, gain_in[None, :], gain_out[None, :],
        gate_weights, up_weights, down_weights,
    )


def device_program(*args):
    tokens, expert_ids = args[:2]
    local_experts = args[5].shape[0]
    all_experts = local_experts * lax.axis_size("ep")
    capacity = max(2, 2 * tokens.shape[0] * expert_ids.shape[1] // all_experts)
    dense = capacity >= tokens.shape[0] and all_experts <= 64
    if dense and (local_experts, lax.axis_size("ep"), lax.axis_size("tp")) == (2, 8, 4):
        return dense_on_device(*args)
    return on_device(*args)


def solution(mesh):
    placed = (
        P("ep", "tp"),
        P("ep", None),
        P("ep", None),
        P("tp"),
        P("tp"),
        P("ep", "tp", None),
        P("ep", "tp", None),
        P("ep", None, "tp"),
    )
    return jax.shard_map(
        device_program, mesh=mesh, in_specs=placed, out_specs=P("ep", "tp"), check_vma=False
    )
```
